32 devices in a mesh: ep: 8 (over z, y), tp: 4 (over x, core).
Axes of the slice: x: 2, y: 2, z: 4, core: 2. Of those that a mesh axis runs over, the one named last changes fastest.
Arguments:
- tokens_first: bfloat16 [4096, 2048], P('ep'), may hold values from -6 to 6
- norm_gain_first: float32 [2048], replicated, may hold values from 0.1 to 1.9
- w_query: bfloat16 [2048, 512], P(None, 'tp'), may hold values from -0.125 to 0.125
- w_key: bfloat16 [2048, 512], P(None, 'tp'), may hold values from -0.125 to 0.125
- w_value: bfloat16 [2048, 1024], P(None, 'tp'), may hold values from -0.125 to 0.125
- w_outgate: bfloat16 [2048, 1024], P(None, 'tp'), may hold values from -0.125 to 0.125
- w_decay: bfloat16 [2048, 512], P(None, 'tp'), may hold values from -1 to 1
- decay_bias: float32 [64, 512], P('ep', 'tp'), may hold values from -1.3 to 12.5
- head_gain: float32 [1024], P('tp'), may hold values from 0.1 to 1.9
- w_mix_out: bfloat16 [1024, 2048], P('tp'), may hold values from -0.1875 to 0.1875
- tokens_second: bfloat16 [2048, 2048], P('ep'), may hold values from -6 to 6
- norm_gain_second: float32 [2048], replicated, may hold values from 0.1 to 1.9
- routes: int32 [2048, 2], P('ep'), may hold values from 0 to 7, all different within a row; in each aligned block of 256 rows (0 to 255, 256 to 511, ...) at most 128 rows name the same one
- route_logits: float32 [2048, 2], P('ep'), may hold values from -8 to 8
- expert_gate: bfloat16 [8, 2048, 3072], P('ep', None, 'tp'), may hold values from -0.125 to 0.125
- expert_up: bfloat16 [8, 2048, 3072], P('ep', None, 'tp'), may hold values from -0.125 to 0.125
- expert_down: bfloat16 [8, 3072, 2048], P('ep', 'tp'), may hold values from -0.109375 to 0.109375
Outputs:
- mixed_first: bfloat16 [4096, 2048], P(('ep', 'tp'))
- mixed_second: bfloat16 [2048, 2048], P('ep', 'tp')
The draws below stay inside these ranges and needn't reach their ends.
Inputs may be any that keep to these rules, and one draw needn't show every extreme that they name: In the rows of one index of ep (aligned blocks of 256 rows) no expert is named by more than 128 rows, a bound that some block reaches; the two routes of a row name different experts.
All inputs are finite; a program needn't handle non-finite values.
Results may differ from the reference program's by a relative error of at most 0.01.
Values may be sent and summed in bfloat16 or wider, within the bound.
A program may use at most 128 MiB of HBM per device.

```python
import math
import jax
import jax.numpy as jnp
import numpy as np
from jax import lax

D = 2048
HEADS = 8
KEY_DIM = 64
VALUE_DIM = 128
FFE = 3072
TOPK = 2
BLOCK = 64
ROWS_B = 256
QK_WIDTH = 512
V_WIDTH = 1024
EXPERTS = 8
TOKENS_A = 4096
TOKENS_B = 2048
NBLK = 64
CAP = 128
N_EP = 8
N_TP = 4


def draw_w_decay(key, part):
    limit = jnp.minimum(15.0 / jnp.sqrt(jnp.float32(D)), jnp.float32(1.0))
    entries = jax.random.normal(jax.random.fold_in(key, 11), (D, QK_WIDTH), jnp.float32) * (2.5 / jnp.sqrt(jnp.float32(D)))
    entries = jnp.clip(entries, -limit, limit)
    return entries.astype(jnp.bfloat16)


def draw_decay_bias(key, part):
    pick_key, slow_key, fast_key, block_key = jax.random.split(key, 4)
    slow_share = 0.5
    chosen = jax.random.uniform(pick_key, (QK_WIDTH,), jnp.float32) < slow_share
    slow_center = jnp.log(jnp.float32(0.86) * TOKENS_A)
    slow_base = slow_center + jax.random.uniform(slow_key, (QK_WIDTH,), jnp.float32, -0.5, 0.5)
    fast_base = jax.random.uniform(fast_key, (QK_WIDTH,), jnp.float32, -0.5, 1.5)
    channel_base = jnp.where(chosen, slow_base, fast_base)
    offset = jax.random.uniform(block_key, (NBLK, 1), jnp.float32, -0.8, 0.8)
    return (channel_base[None, :] + offset).astype(jnp.float32)


def block_scale(key, dims, pieces, smallest, high):
    level, own = 1.0, jax.random.fold_in(key, 6)
    for position, blocks in pieces:
        steps = jnp.exp(jax.random.uniform(jax.random.fold_in(own, position), (blocks,), jnp.float32, smallest / len(pieces), high / len(pieces)))
        level = level * jnp.repeat(steps, dims[position] // blocks).reshape([-1 if axis == position else 1 for axis in range(len(dims))])
    return level


def shared_out(own_key, own, number, rows, amount, top, bound, skew):
    order = jax.random.permutation(own_key, amount)
    crowded, common = portions_of(amount, rows * top, bound, skew, True), portions_of(amount, rows * top, bound, skew, False)
    places = jnp.arange(amount)

    def named(tallies, turn):
        used = int((tallies > 0).sum())
        fixed = max(1, used // 4)
        passed = fixed + (places - fixed + turn * (used - fixed)) % max(1, amount - fixed)
        return jnp.zeros((amount,), jnp.int32).at[order[jnp.where(places < fixed, places, passed)]].set(jnp.asarray(tallies, jnp.int32))

    tallies = jnp.where(number % 4 == 0, named(crowded, number // 4), named(common, number - number // 4 - 1))
    mixed = jax.random.permutation(jax.random.fold_in(own, 3), amount)
    source_of, taker = mixed[0:amount // 2 * 2:2], mixed[1:amount // 2 * 2:2]
    margin = jnp.minimum(tallies[source_of] - 1, bound - tallies[taker]) // 2
    margin = jnp.where((source_of == order[0]) | (taker == order[0]) | (tallies[taker] == 0), 0, jnp.maximum(margin, 0))
    passed = jax.random.randint(jax.random.fold_in(own, 4), (amount // 2,), 0, 1 << 20) % (margin + 1)
    tallies = tallies.at[source_of].add(-passed).at[taker].add(passed)
    labels = jnp.searchsorted(jnp.cumsum(tallies), jnp.arange(rows * top), side="right").astype(jnp.int32)
    grid = labels.reshape(top, rows).T
    grid = grid[jax.random.permutation(jax.random.fold_in(own, 1), rows)]
    turn = jax.random.randint(jax.random.fold_in(own, 2), (rows, 1), 0, top)
    return jnp.take_along_axis(grid, (jnp.arange(top)[None, :] + turn) % top, axis=1)


def portions_of(amount, total, reach, lean, full):
    loads = [(1 << 20) // math.isqrt(grade ** lean) + 1 for grade in range(1, amount + 1)]
    largest = reach if full else min(reach, max(-(-total // amount), total * loads[0] // sum(loads)))
    least = 1 if total - largest >= amount - 1 else 0
    holding, spare = [largest] + [least] * (amount - 1), total - largest - least * (amount - 1)
    while spare > 0:
        movable = [i for i in range(1, amount) if holding[i] < largest] or [i for i in range(1, amount) if holding[i] < reach]
        whole, budget = sum([loads[i] for i in movable]), spare
        for i in movable:
            extra = min(reach - holding[i], max(1, budget * loads[i] // whole), spare)
            holding[i] = holding[i] + extra
            spare = spare - extra
    return np.array(holding)


def gaussian(key, dims, spread, most, cuts=(), held_as=jnp.bfloat16):
    values = spread * jax.random.normal(key, dims, jnp.float32)
    if cuts:
        values = values * block_scale(key, dims, cuts, -0.22, 0.18)
    return jnp.clip(values, -most, most).astype(held_as)


def setup_inputs(seed: int = 0) -> dict:
    splits = jax.random.split(jax.random.key(seed), 18)
    tokens_first = gaussian(splits[0], (TOKENS_A, D), 1.0, 6.0, ((0, 8),))
    norm_gain_first = jnp.clip(1.0 + 0.18 * jax.random.normal(splits[1], (D,), jnp.float32), 0.1, 1.9)
    w_query = gaussian(splits[2], (D, QK_WIDTH), D ** -0.5, 0.125, ((1, 4),))
    w_key = gaussian(splits[3], (D, QK_WIDTH), D ** -0.5, 0.125, ((1, 4),))
    w_value = gaussian(splits[4], (D, V_WIDTH), D ** -0.5, 0.125, ((1, 4),))
    w_outgate = gaussian(splits[5], (D, V_WIDTH), D ** -0.5, 0.125, ((1, 4),))
    w_decay = draw_w_decay(jax.random.fold_in(splits[17], 71), 0)
    decay_bias = draw_decay_bias(jax.random.fold_in(splits[17], 71), 0)
    head_gain = jnp.clip(1.0 + 0.18 * jax.random.normal(splits[8], (V_WIDTH,), jnp.float32), 0.1, 1.9)
    w_mix_out = gaussian(splits[9], (V_WIDTH, D), V_WIDTH ** -0.5, 0.1875, ((0, 4),))
    tokens_second = gaussian(splits[10], (TOKENS_B, D), 1.0, 6.0, ((0, 8),))
    norm_gain_second = jnp.clip(1.0 + 0.18 * jax.random.normal(splits[11], (D,), jnp.float32), 0.1, 1.9)
    routes_keys = jax.random.split(jax.random.fold_in(splits[12], 1), TOKENS_B // ROWS_B)
    routes_turns = jax.random.permutation(jax.random.fold_in(splits[12], 3), TOKENS_B // ROWS_B)
    routes = jax.vmap(lambda own, number: shared_out(jax.random.fold_in(splits[12], 2), own, number, ROWS_B, EXPERTS, TOPK, CAP, 1))(routes_keys, routes_turns).reshape((TOKENS_B, TOPK))
    route_logits = gaussian(splits[13], (TOKENS_B, TOPK), 1.5, 8.0, ((0, 8),), jnp.float32)
    expert_gate = gaussian(splits[14], (EXPERTS, D, FFE), D ** -0.5, 0.125, ((0, 8), (2, 4)))
    expert_up = gaussian(splits[15], (EXPERTS, D, FFE), D ** -0.5, 0.125, ((0, 8), (2, 4)))
    expert_down = gaussian(splits[16], (EXPERTS, FFE, D), FFE ** -0.5, 0.109375, ((0, 8), (1, 4)))
    return dict(tokens_first=tokens_first, norm_gain_first=norm_gain_first, w_query=w_query, w_key=w_key, w_value=w_value, w_outgate=w_outgate, w_decay=w_decay, decay_bias=decay_bias, head_gain=head_gain, w_mix_out=w_mix_out, tokens_second=tokens_second, norm_gain_second=norm_gain_second, routes=routes, route_logits=route_logits, expert_gate=expert_gate, expert_up=expert_up, expert_down=expert_down)


EPS = 1e-06
TEMPER = 16.0

def rms_rows(rows_in, gain_row):
    wide_rows = rows_in.astype(jnp.float32)
    return wide_rows * lax.rsqrt(lax.optimization_barrier(jnp.mean(wide_rows * wide_rows, axis=-1, keepdims=True)) + EPS) * gain_row

def block_step(entry_state, inputs):
    queries, key_rows, value_matrix_rows, log_decay = inputs
    cumul_log = jnp.cumsum(log_decay, axis=0)
    forward_decay_rows = queries * jnp.exp(cumul_log)
    behind = key_rows * jnp.exp(-cumul_log)
    scores = jnp.einsum('thk,shk->hts', forward_decay_rows, behind, precision=lax.Precision.HIGHEST)
    block_len = queries.shape[0]
    causal = jnp.arange(block_len)[:, None] >= jnp.arange(block_len)[None, :]
    scores = jnp.where(causal[None], scores, jnp.zeros_like(scores))
    within = jnp.einsum('hts,shv->thv', scores, value_matrix_rows, precision=lax.Precision.HIGHEST)
    carried_state = jnp.einsum('azm,zmj->azj', forward_decay_rows, entry_state, precision=lax.Precision.HIGHEST)
    final_log_decay = cumul_log[-1]
    fading_factor = key_rows * jnp.exp(final_log_decay[None] - cumul_log)
    following_state = jnp.exp(final_log_decay)[:, :, None] * entry_state + jnp.einsum('drx,drm->rxm', fading_factor, value_matrix_rows, precision=lax.Precision.HIGHEST)
    return (following_state, within + carried_state)

def head_output(attended, out_gate, head_gain):
    scaled = attended * lax.rsqrt(lax.optimization_barrier(jnp.mean(attended * attended, axis=-1, keepdims=True)) + EPS)
    return (scaled.reshape(attended.shape[0], -1) * head_gain * jax.nn.silu(out_gate)).astype(jnp.bfloat16)

def reference(tokens_first, norm_gain_first, w_query, w_key, w_value, w_outgate, w_decay, decay_bias, head_gain, w_mix_out, tokens_second, norm_gain_second, routes, route_logits, expert_gate, expert_up, expert_down):
    normed = rms_rows(tokens_first, norm_gain_first).astype(jnp.bfloat16)
    queries = (jnp.dot(normed, w_query, preferred_element_type=jnp.float32) * KEY_DIM ** (-0.5)).astype(jnp.bfloat16)
    key_rows = jnp.dot(normed, w_key, preferred_element_type=jnp.float32).astype(jnp.bfloat16)
    value_matrix_rows = jnp.dot(normed, w_value, preferred_element_type=jnp.float32).astype(jnp.bfloat16)
    out_gate = jnp.dot(normed, w_outgate, preferred_element_type=jnp.float32)
    decay_pre = jnp.dot(normed, w_decay, preferred_element_type=jnp.float32).reshape(NBLK, BLOCK, QK_WIDTH) + decay_bias[:, None, :]
    log_decay = (jax.nn.log_sigmoid(decay_pre) / TEMPER).reshape(NBLK, BLOCK, HEADS, KEY_DIM)
    queries, key_rows, value_matrix_rows = lax.optimization_barrier((queries, key_rows, value_matrix_rows))
    query_wide = queries.astype(jnp.float32).reshape(NBLK, BLOCK, HEADS, KEY_DIM)
    key_wide = key_rows.astype(jnp.float32).reshape(NBLK, BLOCK, HEADS, KEY_DIM)
    value_wide = value_matrix_rows.astype(jnp.float32).reshape(NBLK, BLOCK, HEADS, VALUE_DIM)
    start_state = jnp.zeros((HEADS, KEY_DIM, VALUE_DIM), jnp.float32)
    _, attended = lax.scan(block_step, start_state, (query_wide, key_wide, value_wide, log_decay))
    attended = attended.reshape(TOKENS_A, HEADS, VALUE_DIM)
    gated_rows = head_output(attended, out_gate, head_gain)
    mixed_first = jnp.dot(gated_rows, w_mix_out, preferred_element_type=jnp.float32).astype(jnp.bfloat16)
    normed_second = rms_rows(tokens_second, norm_gain_second).astype(jnp.bfloat16)
    flat_routes = routes.reshape(-1)
    copies = flat_routes.shape[0]
    slot_room = N_EP * CAP

    def expert_rows(expert_id, collected):
        copy_index = jnp.nonzero(flat_routes == expert_id, size=slot_room, fill_value=copies)[0]
        picked_rows = jnp.take(normed_second, copy_index // TOPK, axis=0, mode='clip')
        gate_out = jnp.dot(picked_rows, expert_gate[expert_id], preferred_element_type=jnp.float32)
        up_out = jnp.dot(picked_rows, expert_up[expert_id], preferred_element_type=jnp.float32)
        hidden = (jax.nn.silu(gate_out) * up_out).astype(jnp.bfloat16)
        hidden_wide = hidden.reshape(slot_room, N_TP, FFE // N_TP).astype(jnp.float32)
        down_wide = expert_down[expert_id].reshape(N_TP, FFE // N_TP, D).astype(jnp.float32)
        tp_parts = jnp.einsum('mtf,tfd->tmd', hidden_wide, down_wide).astype(jnp.bfloat16)
        tp_parts = lax.optimization_barrier(tp_parts).astype(jnp.float32)
        result = lax.optimization_barrier(jnp.sum(tp_parts, axis=0)).astype(jnp.bfloat16)
        return collected.at[copy_index].set(result, mode='drop')
    collected = lax.fori_loop(0, EXPERTS, expert_rows, jnp.zeros((copies, D), jnp.bfloat16))
    route_share = jax.nn.sigmoid(route_logits - route_logits[:, ::-1])
    picked = collected.reshape(TOKENS_B, TOPK, D).astype(jnp.float32)
    mixed_second = lax.optimization_barrier(jnp.sum(picked * route_share[:, :, None], axis=1)).astype(jnp.bfloat16)
    return (mixed_first, mixed_second)
```

```python
import functools

import jax
import jax.numpy as jnp
from jax import lax
from jax.experimental import pallas as pl
from jax.experimental.pallas import tpu as pltpu
from jax.sharding import PartitionSpec as P

KEY_DIM = 64
VALUE_DIM = 128
BLOCK = 64
EPS = 1e-06
TEMPER = 16.0
UNITS = 8
DIRECT = 4
DIRECT_OUT = 0
PIECES = 4
LANES = 128

MESH = pl.DeviceIdType.MESH
F32 = jnp.float32
BF16 = jnp.bfloat16


def flip(index, mask):
    bit = 1
    while bit <= mask:
        if mask & bit:
            index = index + bit - 2 * bit * ((index // bit) % 2)
        bit *= 2
    return index


def dot(a, b):
    return jnp.dot(a, b, preferred_element_type=F32)


def dot_t(a, b, dims):
    return lax.dot_general(a, b, (dims, ((), ())), preferred_element_type=F32)


def rms_scale(wide):
    return lax.rsqrt(jnp.mean(wide * wide, axis=-1, keepdims=True) + EPS)


def kernel(
    n_ep,
    n_tp,
    tokens_first,
    gain_first,
    w_query,
    w_key,
    w_value,
    w_outgate,
    w_decay,
    decay_bias,
    head_gain,
    w_mix_out,
    tokens_second,
    gain_second,
    routes_t,
    logits_t,
    e_gate,
    e_up,
    e_down,
    out_first,
    out_second,
    tf,
    wall,
    wm,
    ts,
    eg,
    eu,
    ed,
    normed2,
    normed,
    q_s,
    k_s,
    v_s,
    g_s,
    cum_s,
    state_s,
    st_send,
    fade_send,
    st_recv,
    fade_recv,
    half_send,
    half_recv,
    inc,
    gated,
    mixp,
    mrecv1,
    msend,
    mrecv2,
    slots,
    rows,
    hid,
    part,
    recv1,
    send2,
    recv2,
    result,
    received,
    result_d,
    received_d,
    info,
    keep,
    share_send,
    share_recv,
    load_sem,
    disp_ss,
    disp_rs,
    xf_ss,
    xf_rs,
    cf_ss,
    cf_rs,
    st_ss,
    st_rs,
    fd_ss,
    fd_rs,
    hf_ss,
    hf_rs,
    m1_ss,
    m1_rs,
    m2_ss,
    m2_rs,
    r1_ss,
    r1_rs,
    r2_ss,
    r2_rs,
    ret_ss,
    ret_rs,
    sh_ss,
    sh_rs,
):
    e = lax.axis_index("ep")
    t = lax.axis_index("tp")
    lo = t % 2
    hi = t // 2
    near = flip(t, 1)
    far = flip(t, 2)
    hi_other = 1 - hi
    near_lo = 1 - lo
    keys = k_s.shape[1]
    values = v_s.shape[1]

    loads = [
        pltpu.make_async_copy(src, dst, load_sem.at[i])
        for i, (src, dst) in enumerate(
            [
                (tokens_second, ts),
                (tokens_first, tf),
                (w_query, wall.at[:, 0:keys]),
                (w_key, wall.at[:, keys : 2 * keys]),
                (w_value, wall.at[:, 2 * keys : 2 * keys + values]),
                (w_outgate, wall.at[:, 2 * keys + values : 2 * keys + 2 * values]),
                (w_decay, wall.at[:, 2 * keys + 2 * values : 3 * keys + 2 * values]),
                (e_gate, eg),
                (e_up, eu),
                (e_down, ed),
                (w_mix_out, wm),
            ]
        )
    ]
    for load in loads:
        load.start()

    barrier = pltpu.get_barrier_semaphore()
    for j in range(1, n_ep):
        pl.semaphore_signal(barrier, inc=1, device_id=(flip(e, j), t), device_id_type=MESH)
    for peer in (near, far):
        pl.semaphore_signal(barrier, inc=1, device_id=(e, peer), device_id_type=MESH)

    n_rows = ts.shape[0]
    n_slots, width = received.shape
    room = n_slots // n_ep
    per = n_ep // UNITS
    unit_rows = n_slots // UNITS
    direct_slots = DIRECT * unit_rows

    def place(s):
        return pl.ds(pl.multiple_of(s * room, room), room)

    mine = e // per
    half = mine // 4
    inner = half + (mine // 2) % 2 == 1

    def unit(u):
        if u < 4:
            return flip(mine, u)
        mid = half if u < 6 else 1 - half
        return 4 * (1 - half) + 2 * mid + flip(mine % 2, u % 2)

    def chunk_at(u, n):
        m = unit(u) // n
        return pl.ds(pl.multiple_of(m * n * unit_rows, n * unit_rows), n * unit_rows)

    def members(u, n=1):
        return [
            (unit(v) * per + flip(e % per, k))
            for v in range(u, u + n)
            for k in range(per)
            if v > 0 or k > 0
        ]

    def cols_of(b):
        return pl.ds(pl.multiple_of(b * width, width), width)

    def remote(src, dst, ss, rs, dev):
        return pltpu.make_async_remote_copy(
            src_ref=src, dst_ref=dst, send_sem=ss, recv_sem=rs, device_id=dev, device_id_type=MESH
        )

    sends = []

    def launch(copy):
        copy.start()
        sends.append(copy)

    expert_col = lax.broadcasted_iota(jnp.int32, (LANES, n_rows), 0)
    rt = routes_t[...]
    m0 = (expert_col == rt[0:1, :]).astype(F32)
    m1 = (expert_col == rt[1:2, :]).astype(F32)
    r_i = lax.broadcasted_iota(jnp.int32, (n_rows, n_rows), 0)
    c_i = lax.broadcasted_iota(jnp.int32, (n_rows, n_rows), 1)
    before = dot((m0 + m1).astype(BF16), (r_i < c_i).astype(BF16))
    t0 = rt[0:1, :] * room + jnp.sum(m0 * before, axis=0, keepdims=True).astype(jnp.int32)
    t1 = rt[1:2, :] * room + jnp.sum(m1 * before, axis=0, keepdims=True).astype(jnp.int32)
    loads[0].wait()
    wide2 = ts[...].astype(F32)
    normed2[...] = (wide2 * rms_scale(wide2) * gain_second[...]).astype(BF16)

    def picks(start, count):
        slot_id = lax.broadcasted_iota(jnp.int32, (count, n_rows), 0) + start
        return ((slot_id == t0) | (slot_id == t1)).astype(F32).astype(BF16)

    tile = 256
    own_base = (e // (DIRECT * per)) * direct_slots

    def build_far(i, carry):
        start = pl.multiple_of((own_base + direct_slots + i * tile) % n_slots, tile)
        slots[0, pl.ds(start, tile), :] = dot(picks(start, tile), normed2[:, cols_of(t)]).astype(
            BF16
        )
        return carry

    def build_own(i, carry):
        start = pl.multiple_of(own_base + i * tile, tile)
        pick = picks(start, tile)
        for h, b in enumerate((t, far)):
            slots[h, pl.ds(start, tile), :] = dot(pick, normed2[:, cols_of(b)]).astype(BF16)
        return carry

    lax.fori_loop(0, (n_slots - direct_slots) // tile, build_far, 0)
    pl.semaphore_wait(barrier, n_ep + 1)

    def dispatch(s, h, sender):
        b = (t, far)[h]
        return remote(
            slots.at[h, place(s), :],
            rows.at[b, place(e), :],
            disp_ss.at[s, h],
            disp_rs.at[sender, h],
            (s, t),
        )

    straight = [dispatch(s, 0, e) for u in (4, 6) for s in members(u)]
    turning = [dispatch(s, 0, e) for u in (5, 7) for s in members(u)]
    sends.extend(straight + turning)

    @pl.when(inner)
    def _():
        for copy in straight:
            copy.start()

    lax.fori_loop(0, direct_slots // tile, build_own, 0)

    def dispatch_own(*units):
        for u in units:
            for s in members(u):
                for h in range(2):
                    launch(dispatch(s, h, e))

    def dispatch_turning():
        @pl.when(inner)
        def _():
            for copy in turning:
                copy.start()

    dispatch_own(1, 0, 2)

    def dispatch_outer():
        @pl.when(jnp.logical_not(inner))
        def _():
            for copy in straight + turning:
                copy.start()

    own_pick = picks(e * room, room)
    for b in range(n_tp):
        rows[b, place(e), :] = dot(own_pick, normed2[:, b * width : (b + 1) * width]).astype(BF16)

    def near_copy(s, h):
        at = rows.at[(t, far)[h], place(s), :]
        return remote(at, at, cf_ss.at[s, h], cf_rs.at[s, h], (e, near))

    def far_copy(s):
        at = rows.at[t, place(s), :]
        return remote(at, at, xf_ss.at[s], xf_rs.at[s], (e, far))

    def forward_own(u):
        for s in members(u):
            for h in range(2 if u < DIRECT else 1):
                dispatch(e, h, s).wait_recv()
            if u >= DIRECT:
                launch(far_copy(s))
            else:
                launch(near_copy(s, 1))
            launch(near_copy(s, 0))

    def forward_far(u):
        for s in members(u):
            far_copy(s).wait_recv()
            launch(near_copy(s, 1))

    def arrived(u):
        for s in members(u):
            for h in range(2):
                near_copy(s, h).wait_recv()

    n_first = tf.shape[0]
    blocks = n_first // BLOCK
    heads = keys // KEY_DIM
    tri_r = lax.broadcasted_iota(jnp.int32, (BLOCK, BLOCK), 0)
    tri_c = lax.broadcasted_iota(jnp.int32, (BLOCK, BLOCK), 1)
    causal = tri_r >= tri_c
    tri = causal.astype(F32)
    head_of = lax.broadcasted_iota(jnp.int32, (1, keys), 1) // KEY_DIM

    def norm_first():
        loads[1].wait()

        def norm_rows(i, carry):
            at = pl.ds(pl.multiple_of(i * BLOCK, BLOCK), BLOCK)
            wide = tf[at, :].astype(F32)
            normed[at, :] = (wide * rms_scale(wide) * gain_first[...]).astype(BF16)
            return carry

        lax.fori_loop(0, blocks, norm_rows, 0, unroll=2)

    def project():
        for load in loads[2:7]:
            load.wait()
        split = 2 * keys + values
        for start in range(0, n_first, tile):
            at = slice(start, start + tile)
            x = normed[at, :]
            left = dot(x, wall[:, 0:split])
            q_s[at, :] = (left[:, 0:keys] * KEY_DIM ** (-0.5)).astype(BF16)
            k_s[at, :] = left[:, keys : 2 * keys].astype(BF16)
            v_s[at, :] = left[:, 2 * keys : split].astype(BF16)
            right = dot(x, wall[:, split:])
            g_s[at, :] = right[:, 0:values]
            cum_s[at, :] = right[:, values:]

    group = n_ep // 2
    first_half = e < group
    spot = e % group

    def state_copies(k, sender):
        peer = e - spot + flip(spot, k)
        at = flip(spot, k) if sender else spot
        to = spot if sender else flip(spot, k)
        return (
            remote(st_send, st_recv.at[to], st_ss.at[at], st_rs.at[to], (peer, t)),
            remote(fade_send, fade_recv.at[to], fd_ss.at[at], fd_rs.at[to], (peer, t)),
        )

    def local_states():
        inc[...] = jnp.zeros_like(inc)

        def local_pass(b, total):
            at = pl.ds(pl.multiple_of(b * BLOCK, BLOCK), BLOCK)
            pre = cum_s[at, :] + decay_bias[pl.ds(b, 1), :]
            log_decay = (jnp.minimum(pre, 0.0) - jnp.log1p(jnp.exp(-jnp.abs(pre)))) / TEMPER
            cum = jnp.dot(
                tri, log_decay, precision=lax.Precision.HIGHEST, preferred_element_type=F32
            )
            cum_s[at, :] = cum
            last = cum[BLOCK - 1 : BLOCK, :]
            fading = (k_s[at, :].astype(F32) * jnp.exp(last - cum)).astype(BF16)
            full = dot_t(v_s[at, :], fading, ((0,), (0,)))
            add = full[0:VALUE_DIM]
            for h in range(1, heads):
                add = jnp.where(head_of == h, full[h * VALUE_DIM : (h + 1) * VALUE_DIM], add)
            state_s[b] = inc[...]
            inc[...] = inc[...] * jnp.exp(last) + add
            return total + last

        total = lax.fori_loop(0, blocks, local_pass, jnp.zeros((1, keys), F32), unroll=4)
        st_send[...] = inc[...].astype(BF16)
        fade_send[...] = jnp.broadcast_to(jnp.exp(total), fade_send.shape)
        st_recv[spot] = st_send[...]
        fade_recv[spot] = fade_send[...]
        for k in range(1, group):
            for copy in state_copies(k, True):
                launch(copy)

    half_copy = remote(half_send, half_recv, hf_ss.at[0], hf_rs.at[0], (flip(e, group), t))

    def fold(p):
        inc[...] = inc[...] * fade_recv[p, 0:1, :] + st_recv[p].astype(F32)

    def relay_state():
        for k in range(1, group):
            for copy in state_copies(k, False):
                copy.wait_recv()

        @pl.when(first_half)
        def _():
            inc[...] = jnp.zeros_like(inc)
            for p in range(group):
                fold(p)
            half_send[...] = inc[...].astype(BF16)
            half_copy.start()

    def share_table():
        lg = logits_t[...]
        row = lax.broadcasted_iota(jnp.int32, (LANES, n_rows), 0)
        parts = (
            t0.astype(F32),
            t1.astype(F32),
            jax.nn.sigmoid(lg[0:1, :] - lg[1:2, :]),
            jax.nn.sigmoid(lg[1:2, :] - lg[0:1, :]),
        )
        table = jnp.zeros((LANES, n_rows), F32)
        for i, line in enumerate(parts):
            table = jnp.where(row == i, line, table)
        info[...] = table.T

    def shares(u):
        start = unit(u) * unit_rows
        slot = lax.broadcasted_iota(jnp.int32, (n_rows, unit_rows), 1) + start
        slot = slot.astype(F32)
        return (
            jnp.where(slot == info[:, 0:1], info[:, 2:3], 0.0)
            + jnp.where(slot == info[:, 1:2], info[:, 3:4], 0.0)
        ).astype(BF16)

    hidden_width = hid.shape[1]

    def expert_weights():
        for load in loads[7:10]:
            load.wait()

    def experts(u, n):
        at = chunk_at(u, n)
        count = n * unit_rows

        for i in range(hidden_width // tile):
            cols = slice(i * tile, (i + 1) * tile)
            gate = jnp.zeros((count, tile), F32)
            upper = jnp.zeros((count, tile), F32)
            for b in range(n_tp):
                x = rows[b, at, :]
                gate = gate + dot(x, eg[0, b * width : (b + 1) * width, cols])
                upper = upper + dot(x, eu[0, b * width : (b + 1) * width, cols])
            hid[0:count, cols] = (gate * jax.nn.sigmoid(gate) * upper).astype(BF16)
        for b in range(n_tp):
            part[b, at, :] = dot(hid[0:count, :], ed[0, :, b * width : (b + 1) * width]).astype(
                BF16
            )

    r1, r2 = {}, {}

    def send_near(u, n):
        at = chunk_at(u, n)
        r1[u] = [
            remote(
                part.at[2 * h + near_lo, at, :],
                recv1.at[h, at, :],
                r1_ss.at[u, h],
                r1_rs.at[u, h],
                (e, near),
            )
            for h in range(2)
        ]
        for copy in r1[u]:
            launch(copy)

    def sum_far(u, n):
        at = chunk_at(u, n)
        for copy in r1[u]:
            copy.wait_recv()
        send2[at, :] = (
            part[2 * hi_other + lo, at, :].astype(F32) + recv1[hi_other, at, :].astype(F32)
        ).astype(BF16)

    def go_far(*units):
        for v in units:
            at = chunk_at(v, 1)
            r2[v] = remote(send2.at[at, :], recv2.at[at, :], r2_ss.at[v], r2_rs.at[v], (e, far))
            launch(r2[v])

    def send_far(u, n):
        sum_far(u, n)
        go_far(*range(u, u + n))

    def back_copy(s, sender):
        return remote(
            result.at[place(s), :],
            received.at[place(e), :],
            ret_ss.at[s, 0],
            ret_rs.at[sender, 0],
            (s, t),
        )

    def back_copy_d(s, h, sender):
        return remote(
            result_d.at[h, place(s), :],
            received_d.at[h, place(e), :],
            ret_ss.at[s, h],
            ret_rs.at[sender, h],
            (s, t),
        )

    def send_back(u, n):
        at = chunk_at(u, n)
        for v in range(u, u + n):
            r2[v].wait_recv()
        result[at, :] = (
            part[t, at, :].astype(F32)
            + recv1[hi, at, :].astype(F32)
            + recv2[at, :].astype(F32)
        ).astype(BF16)
        for s in members(u, n):
            launch(back_copy(s, e))
        if u == 0:
            received[place(e), :] = result[place(e), :]

    def send_direct(u, n):
        at = chunk_at(u, n)
        for copy in r1[u]:
            copy.wait_recv()
        for h in range(2):
            result_d[h, at, :] = (
                part[2 * h + lo, at, :].astype(F32) + recv1[h, at, :].astype(F32)
            ).astype(BF16)
        for s in members(u, n):
            for h in range(2):
                launch(back_copy_d(s, h, e))
        if u == 0:
            for h in range(2):
                received_d[h, place(e), :] = result_d[h, place(e), :]

    share_copy = remote(share_send, share_recv, sh_ss.at[0], sh_rs.at[0], (e, far))

    def combine_direct():
        for s in members(0, DIRECT_OUT):
            for h in range(2):
                back_copy_d(s, h, s).wait_recv()
        sums = [jnp.zeros((n_rows, width), F32) for _ in range(2)]
        for u in range(DIRECT_OUT):
            weights = shares(u)
            for i, h in enumerate((hi_other, hi)):
                sums[i] = sums[i] + dot(weights, received_d[h, chunk_at(u, 1), :])
        share_send[...] = sums[0].astype(BF16)
        launch(share_copy)
        keep[...] = sums[1]

    def gathered(u):
        for s in members(u):
            back_copy(s, s).wait_recv()
        return dot(shares(u), received[chunk_at(u, 1), :])

    def combine(*units):
        total = gathered(units[0])
        for u in units[1:]:
            total = total + gathered(u)
        if units[0] == 0:
            keep[...] = total
        else:
            keep[...] = keep[...] + total

    def combine_last(u):
        total = keep[...]
        if DIRECT_OUT:
            share_copy.wait_recv()
            total = total + share_recv[...].astype(F32)
        out_second[...] = (total + gathered(u)).astype(BF16)

    def attend():
        inc[...] = jnp.zeros_like(inc)

        @pl.when(jnp.logical_not(first_half))
        def _():
            half_copy.wait_recv()
            inc[...] = half_recv[...].astype(F32)

        for p in range(group - 1):

            @pl.when(spot > p)
            def _():
                fold(p)


        def final_pass(b, before_log):
            at = pl.ds(pl.multiple_of(b * BLOCK, BLOCK), BLOCK)
            cum = cum_s[at, :]
            ahead = (q_s[at, :].astype(F32) * jnp.exp(cum)).astype(BF16)
            behind = (k_s[at, :].astype(F32) * jnp.exp(-cum)).astype(BF16)
            entry = (state_s[b] + inc[...] * jnp.exp(before_log)).astype(BF16)
            for h in range(heads):
                cols = slice(h * VALUE_DIM, (h + 1) * VALUE_DIM)
                own = jnp.where(head_of == h, ahead, jnp.zeros_like(ahead))
                scores = jnp.where(causal, dot_t(own, behind, ((1,), (1,))), 0.0)
                attended = dot(scores.astype(BF16), v_s[at, cols]) + dot_t(
                    own, entry, ((1,), (1,))
                )
                gate = g_s[at, cols]
                gated[at, cols] = (
                    attended
                    * rms_scale(attended)
                    * head_gain[:, cols]
                    * (gate * jax.nn.sigmoid(gate))
                ).astype(BF16)
            return before_log + cum[BLOCK - 1 : BLOCK, :]

        lax.fori_loop(0, blocks, final_pass, jnp.zeros((1, keys), F32), unroll=4)

    mix_rows = n_first // n_tp
    mix1 = [
        remote(mixp.at[2 * h + near_lo], mrecv1.at[h], m1_ss.at[h], m1_rs.at[h], (e, near))
        for h in range(2)
    ]
    piece = mix_rows // PIECES

    def mix2(i):
        at = pl.ds(i * piece, piece)
        return remote(msend.at[at, :], mrecv2.at[at, :], m2_ss.at[i], m2_rs.at[i], (e, far))


    def mix_local():
        loads[10].wait()

        for i in range(n_tp):
            at = slice(i * mix_rows, (i + 1) * mix_rows)
            mixp[i] = dot(gated[at, :], wm[...]).astype(BF16)
        for copy in mix1:
            launch(copy)

    def mix_sum():
        for copy in mix1:
            copy.wait_recv()
        msend[...] = (
            mixp[2 * hi_other + lo].astype(F32) + mrecv1[hi_other].astype(F32)
        ).astype(BF16)

    def mix_far(*pieces):
        for i in pieces:
            launch(mix2(i))

    def mix_last():
        for i in range(PIECES):
            mix2(i).wait_recv()
        out_first[...] = (
            mixp[t].astype(F32) + mrecv1[hi].astype(F32) + mrecv2[...].astype(F32)
        ).astype(BF16)

    norm_first()
    project()
    dispatch_turning()
    dispatch_own(3)
    local_states()
    forward_own(4)
    expert_weights()
    share_table()
    experts(0, 1)
    send_near(0, 1)
    dispatch_outer()
    forward_far(4)
    send_far(0, 1)
    arrived(4)
    experts(4, 1)
    send_near(4, 1)
    forward_own(5)
    forward_own(1)
    forward_own(2)
    send_far(4, 1)
    arrived(2)
    experts(2, 1)
    send_near(2, 1)
    forward_far(5)
    arrived(1)
    experts(1, 1)
    send_near(1, 1)
    forward_own(3)
    arrived(5)
    experts(5, 1)
    send_near(5, 1)
    forward_own(6)
    send_back(4, 1)
    send_far(5, 1)
    send_far(1, 1)
    relay_state()
    arrived(3)
    experts(3, 1)
    send_near(3, 1)
    forward_far(6)
    forward_own(7)
    arrived(6)
    experts(6, 1)
    send_near(6, 1)
    send_far(2, 1)
    send_back(0, 1)
    send_back(5, 1)
    send_far(6, 1)
    attend()
    forward_far(7)
    arrived(7)
    experts(7, 1)
    send_near(7, 1)
    send_back(6, 1)
    send_back(1, 1)
    send_back(2, 1)
    send_far(7, 1)
    send_far(3, 1)
    mix_local()
    mix_sum()
    mix_far(0, 1, 2, 3)
    send_back(7, 1)
    send_back(3, 1)
    combine(0, 1, 2, 3)
    combine(4, 5, 6)
    mix_last()
    combine_last(7)
    for copy in sends:
        copy.wait_send()

    @pl.when(first_half)
    def _():
        half_copy.wait_send()


def hand_over(first, second, out_first, out_second, sems):
    copies = [
        pltpu.make_async_copy(first, out_first, sems.at[0]),
        pltpu.make_async_copy(second, out_second, sems.at[1]),
    ]
    for copy in copies:
        copy.start()
    for copy in copies:
        copy.wait()


def body(
    tokens_first,
    norm_gain_first,
    w_query,
    w_key,
    w_value,
    w_outgate,
    w_decay,
    decay_bias,
    head_gain,
    w_mix_out,
    tokens_second,
    norm_gain_second,
    routes,
    route_logits,
    expert_gate,
    expert_up,
    expert_down,
):
    n_ep = lax.axis_size("ep")
    n_tp = lax.axis_size("tp")
    n_first, model = tokens_first.shape
    n_rows = tokens_second.shape[0]
    room = 2 * routes.shape[1] * n_rows // (n_ep * expert_gate.shape[0])
    n_slots = n_ep * room
    width = model // n_tp
    keys = w_query.shape[1]
    values = w_value.shape[1]
    hidden = expert_gate.shape[2]
    blocks = n_first // BLOCK
    mix_rows = n_first // n_tp
    vmem = pltpu.VMEM
    dma = pltpu.SemaphoreType.DMA

    def like(x):
        return vmem(x.shape, x.dtype)

    whole = pl.BlockSpec(memory_space=pltpu.VMEM)
    away = pl.BlockSpec(memory_space=pl.ANY)
    scratch = [
        like(tokens_first),
        vmem((model, 3 * keys + 2 * values), BF16),
        like(w_mix_out),
        like(tokens_second),
        like(expert_gate),
        like(expert_up),
        like(expert_down),
        vmem((n_rows, model), BF16),
        vmem((n_first, model), BF16),
        vmem((n_first, keys), BF16),
        vmem((n_first, keys), BF16),
        vmem((n_first, values), BF16),
        vmem((n_first, values), F32),
        vmem((n_first, keys), F32),
        vmem((blocks, VALUE_DIM, keys), F32),
        vmem((VALUE_DIM, keys), BF16),
        vmem((8, keys), F32),
        vmem((n_ep // 2, VALUE_DIM, keys), BF16),
        vmem((n_ep // 2, 8, keys), F32),
        vmem((VALUE_DIM, keys), BF16),
        vmem((VALUE_DIM, keys), BF16),
        vmem((VALUE_DIM, keys), F32),
        vmem((n_first, values), BF16),
        vmem((n_tp, mix_rows, model), BF16),
        vmem((2, mix_rows, model), BF16),
        vmem((mix_rows, model), BF16),
        vmem((mix_rows, model), BF16),
        vmem((2, n_slots, width), BF16),
        vmem((n_tp, n_slots, width), BF16),
        vmem((n_slots // 4, hidden), BF16),
        vmem((n_tp, n_slots, width), BF16),
        vmem((2, n_slots, width), BF16),
        vmem((n_slots, width), BF16),
        vmem((n_slots, width), BF16),
        vmem((n_slots, width), BF16),
        vmem((n_slots, width), BF16),
        vmem((2, n_slots, width), BF16),
        vmem((2, n_slots, width), BF16),
        vmem((n_rows, LANES), F32),
        vmem((n_rows, width), F32),
        vmem((n_rows, width), BF16),
        vmem((n_rows, width), BF16),
        dma((11,)),
        dma((n_ep, 2)),
        dma((n_ep, 2)),
        dma((n_ep,)),
        dma((n_ep,)),
        dma((n_ep, 2)),
        dma((n_ep, 2)),
        dma((n_ep // 2,)),
        dma((n_ep // 2,)),
        dma((n_ep // 2,)),
        dma((n_ep // 2,)),
        dma((1,)),
        dma((1,)),
        dma((2,)),
        dma((2,)),
        dma((PIECES,)),
        dma((PIECES,)),
        dma((UNITS, 2)),
        dma((UNITS, 2)),
        dma((UNITS,)),
        dma((UNITS,)),
        dma((n_ep, 2)),
        dma((n_ep, 2)),
        dma((1,)),
        dma((1,)),
    ]
    first, second = pl.pallas_call(
        functools.partial(kernel, n_ep, n_tp),
        out_shape=(vmem((mix_rows, model), BF16), vmem((n_rows, width), BF16)),
        in_specs=[away, whole, away, away, away, away, away, whole, whole, away]
        + [away, whole, whole, whole, away, away, away],
        out_specs=(whole, whole),
        scratch_shapes=scratch,
        compiler_params=pltpu.CompilerParams(
            collective_id=0, has_side_effects=True, vmem_limit_bytes=60 * 1024 * 1024
        ),
    )(
        tokens_first,
        norm_gain_first[None, :],
        w_query,
        w_key,
        w_value,
        w_outgate,
        w_decay,
        decay_bias,
        head_gain[None, :],
        w_mix_out,
        tokens_second,
        norm_gain_second[None, :],
        routes.T,
        route_logits.T,
        expert_gate,
        expert_up,
        expert_down,
    )
    return pl.pallas_call(
        hand_over,
        out_shape=(
            jax.ShapeDtypeStruct((mix_rows, model), BF16),
            jax.ShapeDtypeStruct((n_rows, width), BF16),
        ),
        in_specs=[whole, whole],
        out_specs=(away, away),
        scratch_shapes=[dma((2,))],
    )(
        pltpu.with_memory_space_constraint(first, pltpu.VMEM),
        pltpu.with_memory_space_constraint(second, pltpu.VMEM),
    )


def solution(mesh):
    in_specs = (
        P("ep", None),
        P(),
        P(None, "tp"),
        P(None, "tp"),
        P(None, "tp"),
        P(None, "tp"),
        P(None, "tp"),
        P("ep", "tp"),
        P("tp"),
        P("tp", None),
        P("ep", None),
        P(),
        P("ep", None),
        P("ep", None),
        P("ep", None, "tp"),
        P("ep", None, "tp"),
        P("ep", "tp", None),
    )
    out_specs = (P(("ep", "tp"), None), P("ep", "tp"))
    return jax.shard_map(body, mesh=mesh, in_specs=in_specs, out_specs=out_specs, check_vma=False)
```

```python
import functools

import jax
import jax.numpy as jnp
from jax import lax
from jax.experimental import pallas as pl
from jax.experimental.pallas import tpu as pltpu
from jax.sharding import PartitionSpec as P

KEY_DIM = 64
VALUE_DIM = 128
BLOCK = 64
EPS = 1e-06
TEMPER = 16.0
UNITS = 8
DIRECT = 4
PIECES = 8
LANES = 128

MESH = pl.DeviceIdType.MESH
F32 = jnp.float32
BF16 = jnp.bfloat16


def flip(index, mask):
    bit = 1
    while bit <= mask:
        if mask & bit:
            index = index + bit - 2 * bit * ((index // bit) % 2)
        bit *= 2
    return index


def dot(a, b):
    return jnp.dot(a, b, preferred_element_type=F32)


def dot_t(a, b, dims):
    return lax.dot_general(a, b, (dims, ((), ())), preferred_element_type=F32)


def rms_scale(wide):
    return lax.rsqrt(jnp.mean(wide * wide, axis=-1, keepdims=True) + EPS)


def kernel(
    n_ep,
    n_tp,
    tokens_first,
    gain_first,
    w_query,
    w_key,
    w_value,
    w_outgate,
    w_decay,
    decay_bias,
    head_gain,
    w_mix_out,
    tokens_second,
    gain_second,
    routes_t,
    logits_t,
    e_gate,
    e_up,
    e_down,
    out_first,
    out_second,
    tf,
    wall,
    wm,
    ts,
    eg,
    eu,
    ed,
    normed2,
    normed,
    q_s,
    k_s,
    v_s,
    g_s,
    cum_s,
    state_s,
    st_send,
    fade_send,
    st_recv,
    fade_recv,
    half_send,
    half_recv,
    inc,
    gated,
    mixp,
    mrecv1,
    msend,
    mrecv2,
    slots,
    rows,
    hid,
    part,
    recv1,
    send2,
    recv2,
    result,
    received,
    info,
    keep,
    load_sem,
    disp_ss,
    disp_rs,
    xf_ss,
    xf_rs,
    cf_ss,
    cf_rs,
    st_ss,
    st_rs,
    fd_ss,
    fd_rs,
    hf_ss,
    hf_rs,
    m1_ss,
    m1_rs,
    m2_ss,
    m2_rs,
    r1_ss,
    r1_rs,
    r2_ss,
    r2_rs,
    ret_ss,
    ret_rs,
):
    e = lax.axis_index("ep")
    t = lax.axis_index("tp")
    lo = t % 2
    hi = t // 2
    near = flip(t, 1)
    far = flip(t, 2)
    hi_other = 1 - hi
    near_lo = 1 - lo
    keys = k_s.shape[1]
    values = v_s.shape[1]

    loads = [
        pltpu.make_async_copy(src, dst, load_sem.at[i])
        for i, (src, dst) in enumerate(
            [
                (tokens_second, ts),
                (tokens_first, tf),
                (w_query, wall.at[:, 0:keys]),
                (w_key, wall.at[:, keys : 2 * keys]),
                (w_value, wall.at[:, 2 * keys : 2 * keys + values]),
                (w_outgate, wall.at[:, 2 * keys + values : 2 * keys + 2 * values]),
                (w_decay, wall.at[:, 2 * keys + 2 * values : 3 * keys + 2 * values]),
                (e_gate, eg),
                (e_up, eu),
                (e_down, ed),
                (w_mix_out, wm),
            ]
        )
    ]
    for load in loads:
        load.start()

    barrier = pltpu.get_barrier_semaphore()
    for j in range(1, n_ep):
        pl.semaphore_signal(barrier, inc=1, device_id=(flip(e, j), t), device_id_type=MESH)
    for peer in (near, far):
        pl.semaphore_signal(barrier, inc=1, device_id=(e, peer), device_id_type=MESH)

    n_rows = ts.shape[0]
    n_slots, width = received.shape
    room = n_slots // n_ep
    per = n_ep // UNITS
    unit_rows = n_slots // UNITS
    direct_slots = DIRECT * unit_rows

    def place(s):
        return pl.ds(pl.multiple_of(s * room, room), room)

    mine = e // per
    half = mine // 4
    inner = half + (mine // 2) % 2 == 1

    def unit(u):
        if u < 4:
            return flip(mine, u)
        mid = half if u < 6 else 1 - half
        return 4 * (1 - half) + 2 * mid + flip(mine % 2, u % 2)

    def chunk_at(u, n):
        m = unit(u) // n
        return pl.ds(pl.multiple_of(m * n * unit_rows, n * unit_rows), n * unit_rows)

    def members(u, n=1):
        return [
            (unit(v) * per + flip(e % per, k))
            for v in range(u, u + n)
            for k in range(per)
            if v > 0 or k > 0
        ]

    def cols_of(b):
        return pl.ds(pl.multiple_of(b * width, width), width)

    def remote(src, dst, ss, rs, dev):
        return pltpu.make_async_remote_copy(
            src_ref=src, dst_ref=dst, send_sem=ss, recv_sem=rs, device_id=dev, device_id_type=MESH
        )

    sends = []

    def launch(copy):
        copy.start()
        sends.append(copy)

    expert_col = lax.broadcasted_iota(jnp.int32, (LANES, n_rows), 0)
    rt = routes_t[...]
    m0 = (expert_col == rt[0:1, :]).astype(F32)
    m1 = (expert_col == rt[1:2, :]).astype(F32)
    r_i = lax.broadcasted_iota(jnp.int32, (n_rows, n_rows), 0)
    c_i = lax.broadcasted_iota(jnp.int32, (n_rows, n_rows), 1)
    before = dot((m0 + m1).astype(BF16), (r_i < c_i).astype(BF16))
    t0 = rt[0:1, :] * room + jnp.sum(m0 * before, axis=0, keepdims=True).astype(jnp.int32)
    t1 = rt[1:2, :] * room + jnp.sum(m1 * before, axis=0, keepdims=True).astype(jnp.int32)
    loads[0].wait()
    wide2 = ts[...].astype(F32)
    normed2[...] = (wide2 * rms_scale(wide2) * gain_second[...]).astype(BF16)

    def picks(start, count):
        slot_id = lax.broadcasted_iota(jnp.int32, (count, n_rows), 0) + start
        return ((slot_id == t0) | (slot_id == t1)).astype(F32).astype(BF16)

    tile = 256
    own_base = (e // (DIRECT * per)) * direct_slots

    def build_far(i, carry):
        start = pl.multiple_of((own_base + direct_slots + i * tile) % n_slots, tile)
        slots[0, pl.ds(start, tile), :] = dot(picks(start, tile), normed2[:, cols_of(t)]).astype(
            BF16
        )
        return carry

    def build_own(i, carry):
        start = pl.multiple_of(own_base + i * tile, tile)
        pick = picks(start, tile)
        for h, b in enumerate((t, far)):
            slots[h, pl.ds(start, tile), :] = dot(pick, normed2[:, cols_of(b)]).astype(BF16)
        return carry

    lax.fori_loop(0, (n_slots - direct_slots) // tile, build_far, 0)
    pl.semaphore_wait(barrier, n_ep + 1)

    def dispatch(s, h, sender):
        b = (t, far)[h]
        return remote(
            slots.at[h, place(s), :],
            rows.at[b, place(e), :],
            disp_ss.at[s, h],
            disp_rs.at[sender, h],
            (s, t),
        )

    straight = [dispatch(s, 0, e) for u in (4, 6) for s in members(u)]
    turning = [dispatch(s, 0, e) for u in (5, 7) for s in members(u)]
    sends.extend(straight + turning)

    @pl.when(inner)
    def _():
        for copy in straight:
            copy.start()

    lax.fori_loop(0, direct_slots // tile, build_own, 0)

    def dispatch_own(*units):
        for u in units:
            for s in members(u):
                for h in range(2):
                    launch(dispatch(s, h, e))

    def dispatch_turning():
        @pl.when(inner)
        def _():
            for copy in turning:
                copy.start()

    dispatch_own(1, 0, 2)

    def dispatch_outer():
        @pl.when(jnp.logical_not(inner))
        def _():
            for copy in straight + turning:
                copy.start()

    own_pick = picks(e * room, room)
    for b in range(n_tp):
        rows[b, place(e), :] = dot(own_pick, normed2[:, b * width : (b + 1) * width]).astype(BF16)

    def near_copy(s, h):
        at = rows.at[(t, far)[h], place(s), :]
        return remote(at, at, cf_ss.at[s, h], cf_rs.at[s, h], (e, near))

    def far_copy(s):
        at = rows.at[t, place(s), :]
        i = s % (n_ep // 2)
        return remote(at, at, xf_ss.at[i], xf_rs.at[i], (e, far))

    def forward_own(u):
        for s in members(u):
            for h in range(2 if u < DIRECT else 1):
                dispatch(e, h, s).wait_recv()
            if u >= DIRECT:
                launch(far_copy(s))
            else:
                launch(near_copy(s, 1))
            launch(near_copy(s, 0))

    def forward_far(u):
        for s in members(u):
            far_copy(s).wait_recv()
            launch(near_copy(s, 1))

    def arrived(u):
        for s in members(u):
            for h in range(2):
                near_copy(s, h).wait_recv()

    n_first = tf.shape[0]
    blocks = n_first // BLOCK
    heads = keys // KEY_DIM
    tri_r = lax.broadcasted_iota(jnp.int32, (BLOCK, BLOCK), 0)
    tri_c = lax.broadcasted_iota(jnp.int32, (BLOCK, BLOCK), 1)
    causal = tri_r >= tri_c
    tri = causal.astype(F32)
    head_of = lax.broadcasted_iota(jnp.int32, (1, keys), 1) // KEY_DIM

    def norm_first():
        loads[1].wait()

        def norm_rows(i, carry):
            at = pl.ds(pl.multiple_of(i * BLOCK, BLOCK), BLOCK)
            wide = tf[at, :].astype(F32)
            normed[at, :] = (wide * rms_scale(wide) * gain_first[...]).astype(BF16)
            return carry

        lax.fori_loop(0, blocks, norm_rows, 0, unroll=2)

    def project():
        for load in loads[2:7]:
            load.wait()
        split = 2 * keys + values
        for start in range(0, n_first, tile):
            at = slice(start, start + tile)
            x = normed[at, :]
            left = dot(x, wall[:, 0:split])
            q_s[at, :] = (left[:, 0:keys] * KEY_DIM ** (-0.5)).astype(BF16)
            k_s[at, :] = left[:, keys : 2 * keys].astype(BF16)
            v_s[at, :] = left[:, 2 * keys : split].astype(BF16)
            right = dot(x, wall[:, split:])
            g_s[at, :] = right[:, 0:values]
            cum_s[at, :] = right[:, values:]

    group = n_ep // 2
    first_half = e < group
    spot = e % group

    def state_copies(k, sender):
        peer = e - spot + flip(spot, k)
        at = flip(spot, k) if sender else spot
        to = spot if sender else flip(spot, k)
        return (
            remote(st_send, st_recv.at[to], st_ss.at[at], st_rs.at[to], (peer, t)),
            remote(fade_send, fade_recv.at[to], fd_ss.at[at], fd_rs.at[to], (peer, t)),
        )

    def local_states():
        inc[...] = jnp.zeros_like(inc)

        def local_pass(b, total):
            at = pl.ds(pl.multiple_of(b * BLOCK, BLOCK), BLOCK)
            pre = cum_s[at, :] + decay_bias[pl.ds(b, 1), :]
            log_decay = (jnp.minimum(pre, 0.0) - jnp.log1p(jnp.exp(-jnp.abs(pre)))) / TEMPER
            cum = jnp.dot(
                tri, log_decay, precision=lax.Precision.HIGHEST, preferred_element_type=F32
            )
            cum_s[at, :] = cum
            last = cum[BLOCK - 1 : BLOCK, :]
            fading = (k_s[at, :].astype(F32) * jnp.exp(last - cum)).astype(BF16)
            full = dot_t(v_s[at, :], fading, ((0,), (0,)))
            add = full[0:VALUE_DIM]
            for h in range(1, heads):
                add = jnp.where(head_of == h, full[h * VALUE_DIM : (h + 1) * VALUE_DIM], add)
            state_s[b] = inc[...]
            inc[...] = inc[...] * jnp.exp(last) + add
            return total + last

        total = lax.fori_loop(0, blocks, local_pass, jnp.zeros((1, keys), F32), unroll=4)
        st_send[...] = inc[...].astype(BF16)
        fade_send[...] = jnp.broadcast_to(jnp.exp(total), fade_send.shape)
        st_recv[spot] = st_send[...]
        fade_recv[spot] = fade_send[...]
        for k in range(1, group):
            for copy in state_copies(k, True):
                launch(copy)

    half_copy = remote(half_send, half_recv, hf_ss.at[0], hf_rs.at[0], (flip(e, group), t))

    def fold(p):
        inc[...] = inc[...] * fade_recv[p, 0:1, :] + st_recv[p].astype(F32)

    def relay_state():
        for k in range(1, group):
            for copy in state_copies(k, False):
                copy.wait_recv()

        @pl.when(first_half)
        def _():
            inc[...] = jnp.zeros_like(inc)
            for p in range(group):
                fold(p)
            half_send[...] = inc[...].astype(BF16)
            half_copy.start()

    def share_table():
        lg = logits_t[...]
        row = lax.broadcasted_iota(jnp.int32, (LANES, n_rows), 0)
        parts = (
            t0.astype(F32),
            t1.astype(F32),
            jax.nn.sigmoid(lg[0:1, :] - lg[1:2, :]),
            jax.nn.sigmoid(lg[1:2, :] - lg[0:1, :]),
        )
        table = jnp.zeros((LANES, n_rows), F32)
        for i, line in enumerate(parts):
            table = jnp.where(row == i, line, table)
        info[...] = table.T

    def shares(u):
        start = unit(u) * unit_rows
        slot = lax.broadcasted_iota(jnp.int32, (n_rows, unit_rows), 1) + start
        slot = slot.astype(F32)
        return (
            jnp.where(slot == info[:, 0:1], info[:, 2:3], 0.0)
            + jnp.where(slot == info[:, 1:2], info[:, 3:4], 0.0)
        ).astype(BF16)

    hidden_width = hid.shape[1]

    def expert_weights():
        for load in loads[7:10]:
            load.wait()

    def experts(u, n):
        at = chunk_at(u, n)
        count = n * unit_rows

        for i in range(hidden_width // tile):
            cols = slice(i * tile, (i + 1) * tile)
            gate = jnp.zeros((count, tile), F32)
            upper = jnp.zeros((count, tile), F32)
            for b in range(n_tp):
                x = rows[b, at, :]
                gate = gate + dot(x, eg[0, b * width : (b + 1) * width, cols])
                upper = upper + dot(x, eu[0, b * width : (b + 1) * width, cols])
            hid[0:count, cols] = (gate * jax.nn.sigmoid(gate) * upper).astype(BF16)
        for b in range(n_tp):
            part[b // 2, b % 2, at, :] = dot(hid[0:count, :], ed[0, :, b * width : (b + 1) * width]).astype(
                BF16
            )

    r1, r2 = {}, {}

    def send_near(u, n):
        at = chunk_at(u, n)
        r1[u] = remote(
            part.at[:, near_lo, at, :], recv1.at[:, at, :], r1_ss.at[u], r1_rs.at[u], (e, near)
        )
        launch(r1[u])

    def sum_far(u, n):
        at = chunk_at(u, n)
        r1[u].wait_recv()
        send2[at, :] = (
            part[hi_other, lo, at, :].astype(F32) + recv1[hi_other, at, :].astype(F32)
        ).astype(BF16)

    def go_far(*units):
        for v in units:
            at = chunk_at(v, 1)
            r2[v] = remote(send2.at[at, :], recv2.at[at, :], r2_ss.at[v], r2_rs.at[v], (e, far))
            launch(r2[v])

    def send_far(u, n):
        sum_far(u, n)
        go_far(*range(u, u + n))

    def back_copy(s, sender):
        return remote(
            result.at[place(s), :],
            received.at[place(e), :],
            ret_ss.at[s],
            ret_rs.at[sender],
            (s, t),
        )

    def send_back(u, n):
        at = chunk_at(u, n)
        for v in range(u, u + n):
            r2[v].wait_recv()
        result[at, :] = (
            part[hi, lo, at, :].astype(F32)
            + recv1[hi, at, :].astype(F32)
            + recv2[at, :].astype(F32)
        ).astype(BF16)
        for s in members(u, n):
            launch(back_copy(s, e))
        if u == 0:
            received[place(e), :] = result[place(e), :]

    def gathered(u):
        for s in members(u):
            back_copy(s, s).wait_recv()
        return dot(shares(u), received[chunk_at(u, 1), :])

    def combine(*units):
        total = gathered(units[0])
        for u in units[1:]:
            total = total + gathered(u)
        if units[0] == 0:
            keep[...] = total
        else:
            keep[...] = keep[...] + total

    def combine_last(u):
        out_second[...] = (keep[...] + gathered(u)).astype(BF16)

    def attend():
        inc[...] = jnp.zeros_like(inc)

        @pl.when(jnp.logical_not(first_half))
        def _():
            half_copy.wait_recv()
            inc[...] = half_recv[...].astype(F32)

        for p in range(group - 1):

            @pl.when(spot > p)
            def _():
                fold(p)


        def final_pass(b, before_log):
            at = pl.ds(pl.multiple_of(b * BLOCK, BLOCK), BLOCK)
            cum = cum_s[at, :]
            ahead = (q_s[at, :].astype(F32) * jnp.exp(cum)).astype(BF16)
            behind = (k_s[at, :].astype(F32) * jnp.exp(-cum)).astype(BF16)
            entry = (state_s[b] + inc[...] * jnp.exp(before_log)).astype(BF16)
            for h in range(heads):
                cols = slice(h * VALUE_DIM, (h + 1) * VALUE_DIM)
                own = jnp.where(head_of == h, ahead, jnp.zeros_like(ahead))
                scores = jnp.where(causal, dot_t(own, behind, ((1,), (1,))), 0.0)
                attended = dot(scores.astype(BF16), v_s[at, cols]) + dot_t(
                    own, entry, ((1,), (1,))
                )
                gate = g_s[at, cols]
                gated[at, cols] = (
                    attended
                    * rms_scale(attended)
                    * head_gain[:, cols]
                    * (gate * jax.nn.sigmoid(gate))
                ).astype(BF16)
            return before_log + cum[BLOCK - 1 : BLOCK, :]

        lax.fori_loop(0, blocks, final_pass, jnp.zeros((1, keys), F32), unroll=4)

    mix_rows = n_first // n_tp
    mix1 = remote(mixp.at[:, near_lo], mrecv1, m1_ss.at[0], m1_rs.at[0], (e, near))
    piece = mix_rows // PIECES

    def mix2(i):
        at = pl.ds(0, piece) if i == 0 else pl.ds(piece, mix_rows - piece)
        return remote(msend.at[at, :], mrecv2.at[at, :], m2_ss.at[i], m2_rs.at[i], (e, far))


    def mix_local():
        loads[10].wait()

        for i in range(n_tp):
            at = slice(i * mix_rows, (i + 1) * mix_rows)
            mixp[i // 2, i % 2] = dot(gated[at, :], wm[...]).astype(BF16)
        launch(mix1)

    def mix_sum():
        mix1.wait_recv()
        msend[...] = (
            mixp[hi_other, lo].astype(F32) + mrecv1[hi_other].astype(F32)
        ).astype(BF16)

    def mix_far(*pieces):
        for i in pieces:
            launch(mix2(i))

    def mix_last():
        for i in range(2):
            mix2(i).wait_recv()
        out_first[...] = (
            mixp[hi, lo].astype(F32) + mrecv1[hi].astype(F32) + mrecv2[...].astype(F32)
        ).astype(BF16)

    norm_first()
    project()
    dispatch_turning()
    local_states()
    dispatch_own(3)
    forward_own(4)
    expert_weights()
    share_table()
    experts(0, 1)
    send_near(0, 1)
    dispatch_outer()
    forward_far(4)
    send_far(0, 1)
    arrived(4)
    experts(4, 1)
    send_near(4, 1)
    forward_own(5)
    forward_own(2)
    send_far(4, 1)
    arrived(2)
    experts(2, 1)
    send_near(2, 1)
    forward_far(5)
    relay_state()
    forward_own(1)
    send_far(2, 1)
    arrived(5)
    experts(5, 1)
    send_near(5, 1)
    send_back(4, 1)
    arrived(1)
    experts(1, 1)
    send_near(1, 1)
    send_far(5, 1)
    forward_own(6)
    forward_own(3)
    send_far(1, 1)
    arrived(3)
    experts(3, 1)
    send_near(3, 1)
    forward_far(6)
    send_back(5, 1)
    send_back(0, 1)
    forward_own(7)
    send_far(3, 1)
    arrived(6)
    experts(6, 1)
    send_near(6, 1)
    attend()
    send_far(6, 1)
    mix_local()
    send_back(2, 1)
    forward_far(7)
    send_back(1, 1)
    arrived(7)
    experts(7, 1)
    send_near(7, 1)
    mix_sum()
    mix_far(0)
    send_back(3, 1)
    send_far(7, 1)
    mix_far(1)
    send_back(6, 1)
    send_back(7, 1)
    combine(0, 1, 2, 3)
    combine(4, 5, 6)
    combine_last(7)
    mix_last()
    for copy in sends:
        copy.wait_send()

    @pl.when(first_half)
    def _():
        half_copy.wait_send()


def hand_over(first, second, out_first, out_second, sems):
    copies = [
        pltpu.make_async_copy(first, out_first, sems.at[0]),
        pltpu.make_async_copy(second, out_second, sems.at[1]),
    ]
    for copy in copies:
        copy.start()
    for copy in copies:
        copy.wait()


def body(
    tokens_first,
    norm_gain_first,
    w_query,
    w_key,
    w_value,
    w_outgate,
    w_decay,
    decay_bias,
    head_gain,
    w_mix_out,
    tokens_second,
    norm_gain_second,
    routes,
    route_logits,
    expert_gate,
    expert_up,
    expert_down,
):
    n_ep = lax.axis_size("ep")
    n_tp = lax.axis_size("tp")
    n_first, model = tokens_first.shape
    n_rows = tokens_second.shape[0]
    room = 2 * routes.shape[1] * n_rows // (n_ep * expert_gate.shape[0])
    n_slots = n_ep * room
    width = model // n_tp
    keys = w_query.shape[1]
    values = w_value.shape[1]
    hidden = expert_gate.shape[2]
    blocks = n_first // BLOCK
    mix_rows = n_first // n_tp
    vmem = pltpu.VMEM
    dma = pltpu.SemaphoreType.DMA

    def like(x):
        return vmem(x.shape, x.dtype)

    whole = pl.BlockSpec(memory_space=pltpu.VMEM)
    away = pl.BlockSpec(memory_space=pl.ANY)
    scratch = [
        like(tokens_first),
        vmem((model, 3 * keys + 2 * values), BF16),
        like(w_mix_out),
        like(tokens_second),
        like(expert_gate),
        like(expert_up),
        like(expert_down),
        vmem((n_rows, model), BF16),
        vmem((n_first, model), BF16),
        vmem((n_first, keys), BF16),
        vmem((n_first, keys), BF16),
        vmem((n_first, values), BF16),
        vmem((n_first, values), F32),
        vmem((n_first, keys), F32),
        vmem((blocks, VALUE_DIM, keys), F32),
        vmem((VALUE_DIM, keys), BF16),
        vmem((8, keys), F32),
        vmem((n_ep // 2, VALUE_DIM, keys), BF16),
        vmem((n_ep // 2, 8, keys), F32),
        vmem((VALUE_DIM, keys), BF16),
        vmem((VALUE_DIM, keys), BF16),
        vmem((VALUE_DIM, keys), F32),
        vmem((n_first, values), BF16),
        vmem((2, 2, mix_rows, model), BF16),
        vmem((2, mix_rows, model), BF16),
        vmem((mix_rows, model), BF16),
        vmem((mix_rows, model), BF16),
        vmem((2, n_slots, width), BF16),
        vmem((n_tp, n_slots, width), BF16),
        vmem((n_slots // 4, hidden), BF16),
        vmem((2, 2, n_slots, width), BF16),
        vmem((2, n_slots, width), BF16),
        vmem((n_slots, width), BF16),
        vmem((n_slots, width), BF16),
        vmem((n_slots, width), BF16),
        vmem((n_slots, width), BF16),
        vmem((n_rows, LANES), F32),
        vmem((n_rows, width), F32),
        dma((11,)),
        dma((n_ep, 2)),
        dma((n_ep, 2)),
        dma((n_ep // 2,)),
        dma((n_ep // 2,)),
        dma((n_ep, 2)),
        dma((n_ep, 2)),
        dma((n_ep // 2,)),
        dma((n_ep // 2,)),
        dma((n_ep // 2,)),
        dma((n_ep // 2,)),
        dma((1,)),
        dma((1,)),
        dma((1,)),
        dma((1,)),
        dma((2,)),
        dma((2,)),
        dma((UNITS,)),
        dma((UNITS,)),
        dma((UNITS,)),
        dma((UNITS,)),
        dma((n_ep,)),
        dma((n_ep,)),
    ]
    first, second = pl.pallas_call(
        functools.partial(kernel, n_ep, n_tp),
        out_shape=(vmem((mix_rows, model), BF16), vmem((n_rows, width), BF16)),
        in_specs=[away, whole, away, away, away, away, away, whole, whole, away]
        + [away, whole, whole, whole, away, away, away],
        out_specs=(whole, whole),
        scratch_shapes=scratch,
        compiler_params=pltpu.CompilerParams(
            collective_id=0, has_side_effects=True, vmem_limit_bytes=60 * 1024 * 1024
        ),
    )(
        tokens_first,
        norm_gain_first[None, :],
        w_query,
        w_key,
        w_value,
        w_outgate,
        w_decay,
        decay_bias,
        head_gain[None, :],
        w_mix_out,
        tokens_second,
        norm_gain_second[None, :],
        routes.T,
        route_logits.T,
        expert_gate,
        expert_up,
        expert_down,
    )
    return pl.pallas_call(
        hand_over,
        out_shape=(
            jax.ShapeDtypeStruct((mix_rows, model), BF16),
            jax.ShapeDtypeStruct((n_rows, width), BF16),
        ),
        in_specs=[whole, whole],
        out_specs=(away, away),
        scratch_shapes=[dma((2,))],
    )(
        pltpu.with_memory_space_constraint(first, pltpu.VMEM),
        pltpu.with_memory_space_constraint(second, pltpu.VMEM),
    )


def solution(mesh):
    in_specs = (
        P("ep", None),
        P(),
        P(None, "tp"),
        P(None, "tp"),
        P(None, "tp"),
        P(None, "tp"),
        P(None, "tp"),
        P("ep", "tp"),
        P("tp"),
        P("tp", None),
        P("ep", None),
        P(),
        P("ep", None),
        P("ep", None),
        P("ep", None, "tp"),
        P("ep", None, "tp"),
        P("ep", "tp", None),
    )
    out_specs = (P(("ep", "tp"), None), P("ep", "tp"))
    return jax.shard_map(body, mesh=mesh, in_specs=in_specs, out_specs=out_specs, check_vma=False)
```

```python
import functools

import jax
import jax.numpy as jnp
from jax import lax
from jax.experimental import pallas as pl
from jax.experimental.pallas import tpu as pltpu
from jax.sharding import PartitionSpec as P

KEY_DIM = 64
VALUE_DIM = 128
BLOCK = 64
EPS = 1e-06
TEMPER = 16.0
UNITS = 8
DIRECT = 4
PIECES = 8
LANES = 128

MESH = pl.DeviceIdType.MESH
F32 = jnp.float32
BF16 = jnp.bfloat16


def flip(index, mask):
    bit = 1
    while bit <= mask:
        if mask & bit:
            index = index + bit - 2 * bit * ((index // bit) % 2)
        bit *= 2
    return index


def dot(a, b):
    return jnp.dot(a, b, preferred_element_type=F32)


def dot_t(a, b, dims):
    return lax.dot_general(a, b, (dims, ((), ())), preferred_element_type=F32)


def rms_scale(wide):
    return lax.rsqrt(jnp.mean(wide * wide, axis=-1, keepdims=True) + EPS)


def kernel(
    n_ep,
    n_tp,
    tokens_first,
    gain_first,
    w_query,
    w_key,
    w_value,
    w_outgate,
    w_decay,
    decay_bias,
    head_gain,
    w_mix_out,
    tokens_second,
    gain_second,
    routes_t,
    logits_t,
    e_gate,
    e_up,
    e_down,
    out_first,
    out_second,
    tf,
    wall,
    wm,
    ts,
    eg,
    eu,
    ed,
    normed2,
    normed,
    q_s,
    k_s,
    v_s,
    g_s,
    cum_s,
    state_s,
    st_send,
    fade_send,
    st_recv,
    fade_recv,
    half_send,
    half_recv,
    inc,
    gated,
    mixp,
    mrecv1,
    msend,
    mrecv2,
    slots,
    rows,
    hid,
    part,
    recv1,
    send2,
    recv2,
    result,
    received,
    info,
    keep,
    load_sem,
    disp_ss,
    disp_rs,
    xf_ss,
    xf_rs,
    cf_ss,
    cf_rs,
    st_ss,
    st_rs,
    fd_ss,
    fd_rs,
    hf_ss,
    hf_rs,
    m1_ss,
    m1_rs,
    m2_ss,
    m2_rs,
    r1_ss,
    r1_rs,
    r2_ss,
    r2_rs,
    ret_ss,
    ret_rs,
):
    e = lax.axis_index("ep")
    t = lax.axis_index("tp")
    lo = t % 2
    hi = t // 2
    near = flip(t, 1)
    far = flip(t, 2)
    hi_other = 1 - hi
    near_lo = 1 - lo
    keys = k_s.shape[1]
    values = v_s.shape[1]

    loads = [
        pltpu.make_async_copy(src, dst, load_sem.at[i])
        for i, (src, dst) in enumerate(
            [
                (tokens_second, ts),
                (tokens_first, tf),
                (w_query, wall.at[:, 0:keys]),
                (w_key, wall.at[:, keys : 2 * keys]),
                (w_value, wall.at[:, 2 * keys : 2 * keys + values]),
                (w_outgate, wall.at[:, 2 * keys + values : 2 * keys + 2 * values]),
                (w_decay, wall.at[:, 2 * keys + 2 * values : 3 * keys + 2 * values]),
                (e_gate, eg),
                (e_up, eu),
                (e_down, ed),
                (w_mix_out, wm),
            ]
        )
    ]
    for load in loads:
        load.start()

    barrier = pltpu.get_barrier_semaphore()
    for j in range(1, n_ep):
        pl.semaphore_signal(barrier, inc=1, device_id=(flip(e, j), t), device_id_type=MESH)
    for peer in (near, far):
        pl.semaphore_signal(barrier, inc=1, device_id=(e, peer), device_id_type=MESH)

    n_rows = ts.shape[0]
    n_slots, width = received.shape
    room = n_slots // n_ep
    per = n_ep // UNITS
    unit_rows = n_slots // UNITS
    direct_slots = DIRECT * unit_rows

    def place(s):
        return pl.ds(pl.multiple_of(s * room, room), room)

    mine = e // per
    half = mine // 4
    inner = half + (mine // 2) % 2 == 1

    def unit(u):
        if u < 4:
            return flip(mine, u)
        mid = half if u < 6 else 1 - half
        return 4 * (1 - half) + 2 * mid + flip(mine % 2, u % 2)

    def chunk_at(u, n):
        m = unit(u) // n
        return pl.ds(pl.multiple_of(m * n * unit_rows, n * unit_rows), n * unit_rows)

    def members(u, n=1):
        return [
            (unit(v) * per + flip(e % per, k))
            for v in range(u, u + n)
            for k in range(per)
            if v > 0 or k > 0
        ]

    def cols_of(b):
        return pl.ds(pl.multiple_of(b * width, width), width)

    def remote(src, dst, ss, rs, dev):
        return pltpu.make_async_remote_copy(
            src_ref=src, dst_ref=dst, send_sem=ss, recv_sem=rs, device_id=dev, device_id_type=MESH
        )

    sends = []

    def launch(copy):
        copy.start()
        sends.append(copy)

    expert_col = lax.broadcasted_iota(jnp.int32, (LANES, n_rows), 0)
    rt = routes_t[...]
    m0 = (expert_col == rt[0:1, :]).astype(F32)
    m1 = (expert_col == rt[1:2, :]).astype(F32)
    r_i = lax.broadcasted_iota(jnp.int32, (n_rows, n_rows), 0)
    c_i = lax.broadcasted_iota(jnp.int32, (n_rows, n_rows), 1)
    before = dot((m0 + m1).astype(BF16), (r_i < c_i).astype(BF16))
    t0 = rt[0:1, :] * room + jnp.sum(m0 * before, axis=0, keepdims=True).astype(jnp.int32)
    t1 = rt[1:2, :] * room + jnp.sum(m1 * before, axis=0, keepdims=True).astype(jnp.int32)
    loads[0].wait()
    wide2 = ts[...].astype(F32)
    normed2[...] = (wide2 * rms_scale(wide2) * gain_second[...]).astype(BF16)

    def picks(start, count):
        slot_id = lax.broadcasted_iota(jnp.int32, (count, n_rows), 0) + start
        return ((slot_id == t0) | (slot_id == t1)).astype(F32).astype(BF16)

    tile = 256
    own_base = (e // (DIRECT * per)) * direct_slots

    def build_far(i, carry):
        start = pl.multiple_of((own_base + direct_slots + i * tile) % n_slots, tile)
        slots[0, pl.ds(start, tile), :] = dot(picks(start, tile), normed2[:, cols_of(t)]).astype(
            BF16
        )
        return carry

    def build_own(i, carry):
        start = pl.multiple_of(own_base + i * tile, tile)
        pick = picks(start, tile)
        for h, b in enumerate((t, far)):
            slots[h, pl.ds(start, tile), :] = dot(pick, normed2[:, cols_of(b)]).astype(BF16)
        return carry

    lax.fori_loop(0, (n_slots - direct_slots) // tile, build_far, 0)
    pl.semaphore_wait(barrier, n_ep + 1)

    def dispatch(s, h, sender):
        b = (t, far)[h]
        return remote(
            slots.at[h, place(s), :],
            rows.at[b, place(e), :],
            disp_ss.at[s, h],
            disp_rs.at[sender, h],
            (s, t),
        )

    straight = [dispatch(s, 0, e) for u in (4, 6) for s in members(u)]
    turning = [dispatch(s, 0, e) for u in (5, 7) for s in members(u)]
    sends.extend(straight + turning)

    @pl.when(inner)
    def _():
        for copy in straight:
            copy.start()

    lax.fori_loop(0, direct_slots // tile, build_own, 0)

    def dispatch_own(*units):
        for u in units:
            for s in members(u):
                for h in range(2):
                    launch(dispatch(s, h, e))

    def dispatch_turning():
        @pl.when(inner)
        def _():
            for copy in turning:
                copy.start()

    dispatch_own(1, 0, 2)

    def dispatch_outer():
        @pl.when(jnp.logical_not(inner))
        def _():
            for copy in straight + turning:
                copy.start()

    own_pick = picks(e * room, room)
    for b in range(n_tp):
        rows[b, place(e), :] = dot(own_pick, normed2[:, b * width : (b + 1) * width]).astype(BF16)

    def near_copy(s, h):
        at = rows.at[(t, far)[h], place(s), :]
        return remote(at, at, cf_ss.at[s, h], cf_rs.at[s, h], (e, near))

    def far_copy(s):
        at = rows.at[t, place(s), :]
        i = s % (n_ep // 2)
        return remote(at, at, xf_ss.at[i], xf_rs.at[i], (e, far))

    def forward_own(u):
        for s in members(u):
            for h in range(2 if u < DIRECT else 1):
                dispatch(e, h, s).wait_recv()
            if u >= DIRECT:
                launch(far_copy(s))
            else:
                launch(near_copy(s, 1))
            launch(near_copy(s, 0))

    def forward_far(u):
        for s in members(u):
            far_copy(s).wait_recv()
            launch(near_copy(s, 1))

    def arrived(u):
        for s in members(u):
            for h in range(2):
                near_copy(s, h).wait_recv()

    n_first = tf.shape[0]
    blocks = n_first // BLOCK
    heads = keys // KEY_DIM
    tri_r = lax.broadcasted_iota(jnp.int32, (BLOCK, BLOCK), 0)
    tri_c = lax.broadcasted_iota(jnp.int32, (BLOCK, BLOCK), 1)
    causal = tri_r >= tri_c
    tri = causal.astype(F32)
    head_of = lax.broadcasted_iota(jnp.int32, (1, keys), 1) // KEY_DIM

    def norm_first():
        loads[1].wait()

        def norm_rows(i, carry):
            at = pl.ds(pl.multiple_of(i * BLOCK, BLOCK), BLOCK)
            wide = tf[at, :].astype(F32)
            normed[at, :] = (wide * rms_scale(wide) * gain_first[...]).astype(BF16)
            return carry

        lax.fori_loop(0, blocks, norm_rows, 0, unroll=2)

    def project():
        for load in loads[2:7]:
            load.wait()
        split = 2 * keys + values
        for start in range(0, n_first, tile):
            at = slice(start, start + tile)
            x = normed[at, :]
            left = dot(x, wall[:, 0:split])
            q_s[at, :] = (left[:, 0:keys] * KEY_DIM ** (-0.5)).astype(BF16)
            k_s[at, :] = left[:, keys : 2 * keys].astype(BF16)
            v_s[at, :] = left[:, 2 * keys : split].astype(BF16)
            right = dot(x, wall[:, split:])
            g_s[at, :] = right[:, 0:values]
            cum_s[at, :] = right[:, values:]

    group = n_ep // 2
    first_half = e < group
    spot = e % group

    def state_copies(k, sender):
        peer = e - spot + flip(spot, k)
        at = flip(spot, k) if sender else spot
        to = spot if sender else flip(spot, k)
        return (
            remote(st_send, st_recv.at[to], st_ss.at[at], st_rs.at[to], (peer, t)),
            remote(fade_send, fade_recv.at[to], fd_ss.at[at], fd_rs.at[to], (peer, t)),
        )

    def local_states():
        inc[...] = jnp.zeros_like(inc)

        def local_pass(b, total):
            at = pl.ds(pl.multiple_of(b * BLOCK, BLOCK), BLOCK)
            pre = cum_s[at, :] + decay_bias[pl.ds(b, 1), :]
            log_decay = (jnp.minimum(pre, 0.0) - jnp.log1p(jnp.exp(-jnp.abs(pre)))) / TEMPER
            cum = jnp.dot(
                tri, log_decay, precision=lax.Precision.HIGHEST, preferred_element_type=F32
            )
            cum_s[at, :] = cum
            last = cum[BLOCK - 1 : BLOCK, :]
            fading = (k_s[at, :].astype(F32) * jnp.exp(last - cum)).astype(BF16)
            full = dot_t(v_s[at, :], fading, ((0,), (0,)))
            add = full[0:VALUE_DIM]
            for h in range(1, heads):
                add = jnp.where(head_of == h, full[h * VALUE_DIM : (h + 1) * VALUE_DIM], add)
            state_s[b] = inc[...]
            inc[...] = inc[...] * jnp.exp(last) + add
            return total + last

        total = lax.fori_loop(0, blocks, local_pass, jnp.zeros((1, keys), F32), unroll=4)
        st_send[...] = inc[...].astype(BF16)
        fade_send[...] = jnp.broadcast_to(jnp.exp(total), fade_send.shape)
        st_recv[spot] = st_send[...]
        fade_recv[spot] = fade_send[...]
        for k in range(1, group):
            for copy in state_copies(k, True):
                launch(copy)

    half_copy = remote(half_send, half_recv, hf_ss.at[0], hf_rs.at[0], (flip(e, group), t))

    def fold(p):
        inc[...] = inc[...] * fade_recv[p, 0:1, :] + st_recv[p].astype(F32)

    def relay_state():
        for k in range(1, group):
            for copy in state_copies(k, False):
                copy.wait_recv()

        @pl.when(first_half)
        def _():
            inc[...] = jnp.zeros_like(inc)
            for p in range(group):
                fold(p)
            half_send[...] = inc[...].astype(BF16)
            half_copy.start()

    def share_table():
        lg = logits_t[...]
        row = lax.broadcasted_iota(jnp.int32, (LANES, n_rows), 0)
        parts = (
            t0.astype(F32),
            t1.astype(F32),
            jax.nn.sigmoid(lg[0:1, :] - lg[1:2, :]),
            jax.nn.sigmoid(lg[1:2, :] - lg[0:1, :]),
        )
        table = jnp.zeros((LANES, n_rows), F32)
        for i, line in enumerate(parts):
            table = jnp.where(row == i, line, table)
        info[...] = table.T

    def shares(u):
        start = unit(u) * unit_rows
        slot = lax.broadcasted_iota(jnp.int32, (n_rows, unit_rows), 1) + start
        slot = slot.astype(F32)
        return (
            jnp.where(slot == info[:, 0:1], info[:, 2:3], 0.0)
            + jnp.where(slot == info[:, 1:2], info[:, 3:4], 0.0)
        ).astype(BF16)

    hidden_width = hid.shape[1]

    def expert_weights():
        for load in loads[7:10]:
            load.wait()

    def experts(u, n):
        at = chunk_at(u, n)
        count = n * unit_rows

        for i in range(hidden_width // tile):
            cols = slice(i * tile, (i + 1) * tile)
            gate = jnp.zeros((count, tile), F32)
            upper = jnp.zeros((count, tile), F32)
            for b in range(n_tp):
                x = rows[b, at, :]
                gate = gate + dot(x, eg[0, b * width : (b + 1) * width, cols])
                upper = upper + dot(x, eu[0, b * width : (b + 1) * width, cols])
            hid[0:count, cols] = (gate * jax.nn.sigmoid(gate) * upper).astype(BF16)
        for b in range(n_tp):
            part[b // 2, b % 2, at, :] = dot(hid[0:count, :], ed[0, :, b * width : (b + 1) * width]).astype(
                BF16
            )

    r1, r2 = {}, {}

    def send_near(u, n):
        at = chunk_at(u, n)
        r1[u] = remote(
            part.at[:, near_lo, at, :], recv1.at[:, at, :], r1_ss.at[u], r1_rs.at[u], (e, near)
        )
        launch(r1[u])

    def sum_far(u, n):
        at = chunk_at(u, n)
        r1[u].wait_recv()
        send2[at, :] = (
            part[hi_other, lo, at, :].astype(F32) + recv1[hi_other, at, :].astype(F32)
        ).astype(BF16)

    def go_far(*units):
        for v in units:
            at = chunk_at(v, 1)
            r2[v] = remote(send2.at[at, :], recv2.at[at, :], r2_ss.at[v], r2_rs.at[v], (e, far))
            launch(r2[v])

    def send_far(u, n):
        sum_far(u, n)
        go_far(*range(u, u + n))

    def back_copy(s, sender):
        return remote(
            result.at[place(s), :],
            received.at[place(e), :],
            ret_ss.at[s],
            ret_rs.at[sender],
            (s, t),
        )

    def send_back(u, n):
        at = chunk_at(u, n)
        for v in range(u, u + n):
            r2[v].wait_recv()
        result[at, :] = (
            part[hi, lo, at, :].astype(F32)
            + recv1[hi, at, :].astype(F32)
            + recv2[at, :].astype(F32)
        ).astype(BF16)
        for s in members(u, n):
            launch(back_copy(s, e))
        if u == 0:
            received[place(e), :] = result[place(e), :]

    def gathered(u):
        for s in members(u):
            back_copy(s, s).wait_recv()
        return dot(shares(u), received[chunk_at(u, 1), :])

    def combine(*units):
        total = gathered(units[0])
        for u in units[1:]:
            total = total + gathered(u)
        if units[0] == 0:
            keep[...] = total
        else:
            keep[...] = keep[...] + total

    def combine_last(u):
        out_second[...] = (keep[...] + gathered(u)).astype(BF16)

    def attend():
        inc[...] = jnp.zeros_like(inc)

        @pl.when(jnp.logical_not(first_half))
        def _():
            half_copy.wait_recv()
            inc[...] = half_recv[...].astype(F32)

        for p in range(group - 1):

            @pl.when(spot > p)
            def _():
                fold(p)


        def final_pass(b, before_log):
            at = pl.ds(pl.multiple_of(b * BLOCK, BLOCK), BLOCK)
            cum = cum_s[at, :]
            ahead = (q_s[at, :].astype(F32) * jnp.exp(cum)).astype(BF16)
            behind = (k_s[at, :].astype(F32) * jnp.exp(-cum)).astype(BF16)
            entry = (state_s[b] + inc[...] * jnp.exp(before_log)).astype(BF16)
            for h in range(heads):
                cols = slice(h * VALUE_DIM, (h + 1) * VALUE_DIM)
                own = jnp.where(head_of == h, ahead, jnp.zeros_like(ahead))
                scores = jnp.where(causal, dot_t(own, behind, ((1,), (1,))), 0.0)
                attended = dot(scores.astype(BF16), v_s[at, cols]) + dot_t(
                    own, entry, ((1,), (1,))
                )
                gate = g_s[at, cols]
                gated[at, cols] = (
                    attended
                    * rms_scale(attended)
                    * head_gain[:, cols]
                    * (gate * jax.nn.sigmoid(gate))
                ).astype(BF16)
            return before_log + cum[BLOCK - 1 : BLOCK, :]

        lax.fori_loop(0, blocks, final_pass, jnp.zeros((1, keys), F32), unroll=4)

    mix_rows = n_first // n_tp
    mix1 = remote(mixp.at[:, near_lo], mrecv1, m1_ss.at[0], m1_rs.at[0], (e, near))
    piece = mix_rows // PIECES

    def mix2(i):
        at = pl.ds(0, piece) if i == 0 else pl.ds(piece, mix_rows - piece)
        return remote(msend.at[at, :], mrecv2.at[at, :], m2_ss.at[i], m2_rs.at[i], (e, far))


    def mix_local():
        loads[10].wait()

        for i in range(n_tp):
            at = slice(i * mix_rows, (i + 1) * mix_rows)
            mixp[i // 2, i % 2] = dot(gated[at, :], wm[...]).astype(BF16)
        launch(mix1)

    def mix_sum():
        mix1.wait_recv()
        msend[...] = (
            mixp[hi_other, lo].astype(F32) + mrecv1[hi_other].astype(F32)
        ).astype(BF16)

    def mix_far(*pieces):
        for i in pieces:
            launch(mix2(i))

    def mix_last():
        for i in range(2):
            mix2(i).wait_recv()
        out_first[...] = (
            mixp[hi, lo].astype(F32) + mrecv1[hi].astype(F32) + mrecv2[...].astype(F32)
        ).astype(BF16)

    norm_first()
    project()
    dispatch_turning()
    local_states()
    dispatch_own(3)
    forward_own(4)
    expert_weights()
    share_table()
    experts(0, 1)
    send_near(0, 1)
    dispatch_outer()
    forward_far(4)
    send_far(0, 1)
    arrived(4)
    experts(4, 1)
    send_near(4, 1)
    forward_own(5)
    forward_own(2)
    send_far(4, 1)
    arrived(2)
    experts(2, 1)
    send_near(2, 1)
    forward_far(5)
    relay_state()
    forward_own(1)
    send_far(2, 1)
    arrived(5)
    experts(5, 1)
    send_near(5, 1)
    send_back(4, 1)
    arrived(1)
    experts(1, 1)
    send_near(1, 1)
    forward_own(6)
    send_far(5, 1)
    forward_own(3)
    arrived(3)
    experts(3, 1)
    send_near(3, 1)
    forward_far(6)
    forward_own(7)
    send_far(1, 1)
    send_back(0, 1)
    arrived(6)
    experts(6, 1)
    send_near(6, 1)
    send_back(5, 1)
    send_far(3, 1)
    attend()
    send_far(6, 1)
    forward_far(7)
    mix_local()
    send_back(2, 1)
    arrived(7)
    experts(7, 1)
    send_near(7, 1)
    send_back(1, 1)
    mix_sum()
    send_far(7, 1)
    mix_far(0, 1)
    send_back(3, 1)
    send_back(6, 1)
    send_back(7, 1)
    combine(0, 1, 2, 3)
    combine(4, 5, 6)
    combine_last(7)
    mix_last()
    for copy in sends:
        copy.wait_send()

    @pl.when(first_half)
    def _():
        half_copy.wait_send()


def hand_over(first, second, out_first, out_second, sems):
    copies = [
        pltpu.make_async_copy(first, out_first, sems.at[0]),
        pltpu.make_async_copy(second, out_second, sems.at[1]),
    ]
    for copy in copies:
        copy.start()
    for copy in copies:
        copy.wait()


def body(
    tokens_first,
    norm_gain_first,
    w_query,
    w_key,
    w_value,
    w_outgate,
    w_decay,
    decay_bias,
    head_gain,
    w_mix_out,
    tokens_second,
    norm_gain_second,
    routes,
    route_logits,
    expert_gate,
    expert_up,
    expert_down,
):
    n_ep = lax.axis_size("ep")
    n_tp = lax.axis_size("tp")
    n_first, model = tokens_first.shape
    n_rows = tokens_second.shape[0]
    room = 2 * routes.shape[1] * n_rows // (n_ep * expert_gate.shape[0])
    n_slots = n_ep * room
    width = model // n_tp
    keys = w_query.shape[1]
    values = w_value.shape[1]
    hidden = expert_gate.shape[2]
    blocks = n_first // BLOCK
    mix_rows = n_first // n_tp
    vmem = pltpu.VMEM
    dma = pltpu.SemaphoreType.DMA

    def like(x):
        return vmem(x.shape, x.dtype)

    whole = pl.BlockSpec(memory_space=pltpu.VMEM)
    away = pl.BlockSpec(memory_space=pl.ANY)
    scratch = [
        like(tokens_first),
        vmem((model, 3 * keys + 2 * values), BF16),
        like(w_mix_out),
        like(tokens_second),
        like(expert_gate),
        like(expert_up),
        like(expert_down),
        vmem((n_rows, model), BF16),
        vmem((n_first, model), BF16),
        vmem((n_first, keys), BF16),
        vmem((n_first, keys), BF16),
        vmem((n_first, values), BF16),
        vmem((n_first, values), F32),
        vmem((n_first, keys), F32),
        vmem((blocks, VALUE_DIM, keys), F32),
        vmem((VALUE_DIM, keys), BF16),
        vmem((8, keys), F32),
        vmem((n_ep // 2, VALUE_DIM, keys), BF16),
        vmem((n_ep // 2, 8, keys), F32),
        vmem((VALUE_DIM, keys), BF16),
        vmem((VALUE_DIM, keys), BF16),
        vmem((VALUE_DIM, keys), F32),
        vmem((n_first, values), BF16),
        vmem((2, 2, mix_rows, model), BF16),
        vmem((2, mix_rows, model), BF16),
        vmem((mix_rows, model), BF16),
        vmem((mix_rows, model), BF16),
        vmem((2, n_slots, width), BF16),
        vmem((n_tp, n_slots, width), BF16),
        vmem((n_slots // 4, hidden), BF16),
        vmem((2, 2, n_slots, width), BF16),
        vmem((2, n_slots, width), BF16),
        vmem((n_slots, width), BF16),
        vmem((n_slots, width), BF16),
        vmem((n_slots, width), BF16),
        vmem((n_slots, width), BF16),
        vmem((n_rows, LANES), F32),
        vmem((n_rows, width), F32),
        dma((11,)),
        dma((n_ep, 2)),
        dma((n_ep, 2)),
        dma((n_ep // 2,)),
        dma((n_ep // 2,)),
        dma((n_ep, 2)),
        dma((n_ep, 2)),
        dma((n_ep // 2,)),
        dma((n_ep // 2,)),
        dma((n_ep // 2,)),
        dma((n_ep // 2,)),
        dma((1,)),
        dma((1,)),
        dma((1,)),
        dma((1,)),
        dma((2,)),
        dma((2,)),
        dma((UNITS,)),
        dma((UNITS,)),
        dma((UNITS,)),
        dma((UNITS,)),
        dma((n_ep,)),
        dma((n_ep,)),
    ]
    first, second = pl.pallas_call(
        functools.partial(kernel, n_ep, n_tp),
        out_shape=(vmem((mix_rows, model), BF16), vmem((n_rows, width), BF16)),
        in_specs=[away, whole, away, away, away, away, away, whole, whole, away]
        + [away, whole, whole, whole, away, away, away],
        out_specs=(whole, whole),
        scratch_shapes=scratch,
        compiler_params=pltpu.CompilerParams(
            collective_id=0, has_side_effects=True, vmem_limit_bytes=60 * 1024 * 1024
        ),
    )(
        tokens_first,
        norm_gain_first[None, :],
        w_query,
        w_key,
        w_value,
        w_outgate,
        w_decay,
        decay_bias,
        head_gain[None, :],
        w_mix_out,
        tokens_second,
        norm_gain_second[None, :],
        routes.T,
        route_logits.T,
        expert_gate,
        expert_up,
        expert_down,
    )
    return pl.pallas_call(
        hand_over,
        out_shape=(
            jax.ShapeDtypeStruct((mix_rows, model), BF16),
            jax.ShapeDtypeStruct((n_rows, width), BF16),
        ),
        in_specs=[whole, whole],
        out_specs=(away, away),
        scratch_shapes=[dma((2,))],
    )(
        pltpu.with_memory_space_constraint(first, pltpu.VMEM),
        pltpu.with_memory_space_constraint(second, pltpu.VMEM),
    )


def solution(mesh):
    in_specs = (
        P("ep", None),
        P(),
        P(None, "tp"),
        P(None, "tp"),
        P(None, "tp"),
        P(None, "tp"),
        P(None, "tp"),
        P("ep", "tp"),
        P("tp"),
        P("tp", None),
        P("ep", None),
        P(),
        P("ep", None),
        P("ep", None),
        P("ep", None, "tp"),
        P("ep", None, "tp"),
        P("ep", "tp", None),
    )
    out_specs = (P(("ep", "tp"), None), P("ep", "tp"))
    return jax.shard_map(body, mesh=mesh, in_specs=in_specs, out_specs=out_specs, check_vma=False)
```
